32 devices in a mesh: sp: 8 (over z, x), dp: 4 (over y, core).
Axes of the slice: x: 2, y: 2, z: 4, core: 2. Of those that a mesh axis runs over, the one named last changes fastest.
Arguments:
- queries: bfloat16 [16, 8, 512, 256], P('dp', None, 'sp'), may hold values from -6 to 6
- keys: bfloat16 [16, 8, 512, 256], P('dp', None, 'sp'), may hold values from -6 to 6
- values: bfloat16 [16, 8, 512, 256], P('dp', None, 'sp'), may hold values from -6 to 6
- log_decay: float32 [128, 512], P(('dp', 'sp')), may hold values from -2 to 0, as said below
- w_out: bfloat16 [8, 256, 2048], P(None, None, 'dp'), may hold values from -0.125 to 0.125
Outputs:
- mixed_out: bfloat16 [16, 512, 2048], P('dp', 'sp')
The draws below stay inside these ranges and needn't reach their ends.
Inputs may be any that keep to these rules, and one draw needn't show every extreme that they name: Every entry of log_decay is below zero.
All inputs are finite; a program needn't handle non-finite values.
Results may differ from the reference program's by a relative error of at most 0.008.
Values may be sent and summed in bfloat16 or wider, within the bound.
A program may use at most 128 MiB of HBM per device.

```python
import jax
import jax.numpy as jnp
from jax import lax

WIDTH = 2048
HEADS = 8
HEAD_DIM = 256
BLOCK = 64
SEG_DEV = 64
SEQUENCE_LENGTH = 512
SEQUENCE_TOTAL = 16


def draw_log_decay(key, part):
    random_subkeys = jax.random.split(key, 7)
    order = jax.random.permutation(random_subkeys[0], HEADS)
    fast_count = HEADS // 2
    is_fast = order < fast_count
    fast_rate = jax.random.uniform(random_subkeys[1], (HEADS,), jnp.float32, 1.0 / 60.0, 1.0 / 30.0)
    slow_rate = jax.random.uniform(random_subkeys[2], (HEADS,), jnp.float32, 0.1, 0.5) / SEQUENCE_LENGTH
    per_head_rate = jnp.where(is_fast, fast_rate, slow_rate)
    segment_count = SEQUENCE_LENGTH // SEG_DEV
    segment_factor = jnp.exp(jax.random.uniform(random_subkeys[3], (SEQUENCE_TOTAL, segment_count), jnp.float32, jnp.log(0.5), jnp.log(2.0)))
    segment_factor = jnp.repeat(segment_factor, SEG_DEV, axis=1)
    coarse_estimate = jax.random.uniform(random_subkeys[4], (SEQUENCE_TOTAL, HEADS, SEQUENCE_LENGTH), jnp.float32, 0.6, 1.4)
    spike_position = jax.random.randint(random_subkeys[5], (SEQUENCE_TOTAL, 2), 0, SEQUENCE_LENGTH)
    spike_depth = jnp.log(jax.random.uniform(random_subkeys[6], (SEQUENCE_TOTAL, 2), jnp.float32, 0.6, 0.8))
    position_index = jnp.arange(SEQUENCE_LENGTH, dtype=jnp.int32)
    decay_spike = jnp.sum(jnp.where(position_index[None, None, :] == spike_position[:, :, None], spike_depth[:, :, None], 0.0), axis=1)
    final_output = -per_head_rate[None, :, None] * segment_factor[:, None, :] * coarse_estimate + decay_spike[:, None, :]
    return final_output.reshape(SEQUENCE_TOTAL * HEADS, SEQUENCE_LENGTH).astype(jnp.float32)


def steps_of(own_key, dims, pieces, least, largest):
    loudness, own = 1.0, jax.random.fold_in(own_key, 6)
    for axis_at, parts in pieces:
        draws = jnp.exp(jax.random.uniform(jax.random.fold_in(own, axis_at), (parts,), jnp.float32, least / len(pieces), largest / len(pieces)))
        loudness = loudness * jnp.repeat(draws, dims[axis_at] // parts).reshape([-1 if axis == axis_at else 1 for axis in range(len(dims))])
    return loudness


def centred(own_key, dims, scale, bound, shards=(), kind=jnp.bfloat16):
    entries = scale * jax.random.normal(own_key, dims, jnp.float32)
    if shards:
        entries = entries * steps_of(own_key, dims, shards, -0.22, 0.18)
    return jnp.clip(entries, -bound, bound).astype(kind)


def setup_inputs(seed: int = 0) -> dict:
    arg_keys = jax.random.split(jax.random.key(seed), 6)
    queries = centred(arg_keys[0], (SEQUENCE_TOTAL, HEADS, SEQUENCE_LENGTH, HEAD_DIM), 1.0, 6.0, ((0, 4), (2, 8)))
    keys = centred(arg_keys[1], (SEQUENCE_TOTAL, HEADS, SEQUENCE_LENGTH, HEAD_DIM), 1.0, 6.0, ((0, 4), (2, 8)))
    values = centred(arg_keys[2], (SEQUENCE_TOTAL, HEADS, SEQUENCE_LENGTH, HEAD_DIM), 1.0, 6.0, ((0, 4), (2, 8)))
    log_decay = draw_log_decay(jax.random.fold_in(arg_keys[5], 71), 0)
    w_out = centred(arg_keys[4], (HEADS, HEAD_DIM, WIDTH), (HEADS * HEAD_DIM) ** -0.5, 0.125, ((2, 4),))
    return dict(queries=queries, keys=keys, values=values, log_decay=log_decay, w_out=w_out)


def rotate(field_in, cosine, sine_tab):
    half_dim = field_in.shape[1] // 2
    widened = field_in.astype(jnp.float32)
    first_half = widened[:, :half_dim]
    second_half = widened[:, half_dim:]
    turned = jnp.concatenate([first_half * cosine - second_half * sine_tab, second_half * cosine + first_half * sine_tab], axis=1)
    return turned.astype(jnp.bfloat16)

def product(form, left_op, right_op):
    return jnp.einsum(form, left_op.astype(jnp.float32), right_op.astype(jnp.float32), precision=lax.Precision.HIGHEST)

def retain(query_rows, key_rows, value_rows, decay_row, cosine, sine_tab):
    length, head_width = query_rows.shape
    blocks = length // BLOCK
    rot_query = rotate(query_rows, cosine, sine_tab).reshape(blocks, BLOCK, head_width)
    rot_key = rotate(key_rows, cosine, sine_tab).reshape(blocks, BLOCK, head_width)
    value_blocks = value_rows.reshape(blocks, BLOCK, head_width)
    within = jnp.cumsum(decay_row.astype(jnp.float32).reshape(blocks, BLOCK), axis=1)
    ending = within[:, -1:]
    causal = jnp.tril(jnp.ones((BLOCK, BLOCK), dtype=bool))[None]
    spread = within[:, :, None] - within[:, None, :]
    decay_mask = jnp.where(causal, jnp.exp(jnp.where(causal, spread, 0.0)), 0.0)
    scores = product('bnd,bmd->bnm', rot_query, rot_key)
    weights = (scores * decay_mask).astype(jnp.bfloat16)
    scaled_keys = (rot_key.astype(jnp.float32) * jnp.exp(ending - within)[:, :, None]).astype(jnp.bfloat16)
    updates = product('bmd,bme->bde', scaled_keys, value_blocks)

    def advance(state_now, inputs):
        factor, update = inputs
        return (factor * state_now + update, state_now.astype(jnp.bfloat16))
    start_state = jnp.zeros((head_width, head_width), jnp.float32)
    _, before = lax.scan(advance, start_state, (jnp.exp(ending[:, 0]), updates))
    local_part = product('bnm,bme->bne', weights, value_blocks)
    carried = product('bnd,bde->bne', rot_query, before)
    combined = local_part + jnp.exp(within)[:, :, None] * carried
    return combined.reshape(length, head_width).astype(jnp.bfloat16)

def reference(queries, keys, values, log_decay, w_out):
    seq_count, head_count, length, head_width = queries.shape
    item_count = seq_count * head_count
    half_dim = head_width // 2
    frequency = 10000.0 ** (-jnp.arange(half_dim, dtype=jnp.float32) / half_dim)
    angles = jnp.arange(length, dtype=jnp.float32)[:, None] * frequency[None, :]
    cosine = jnp.cos(angles)
    sine_tab = jnp.sin(angles)

    def one_item(inputs):
        return retain(inputs[0], inputs[1], inputs[2], inputs[3], cosine, sine_tab)
    retained = lax.map(one_item, (queries.reshape(item_count, length, head_width), keys.reshape(item_count, length, head_width), values.reshape(item_count, length, head_width), log_decay))
    retained = retained.reshape(seq_count, head_count, length, head_width)

    def project(seq_rows):
        widened = seq_rows.astype(jnp.float32)
        normed = (widened * lax.rsqrt(lax.optimization_barrier(jnp.mean(widened * widened, axis=-1, keepdims=True)) + 1e-06)).astype(jnp.bfloat16)
        return product('htd,hde->te', normed, w_out).astype(jnp.bfloat16)
    return lax.map(project, retained)
```

```python
import functools

import jax
import jax.numpy as jnp
from jax import lax
from jax.experimental import pallas as pl
from jax.experimental.pallas import tpu as pltpu
from jax.sharding import PartitionSpec as P

MESH = pl.DeviceIdType.MESH
F32 = jnp.float32
BF16 = jnp.bfloat16


def kernel(sizes, freq_ref, q_hbm, k_hbm, v_hbm, ld_hbm, w_hbm, out_ref,
           qbuf, kbuf, vbuf, ldbuf, ldrows, cos_tab, sin_tab, wbuf, tin, tout, obuf, xbuf,
           local_sem, ld_send, ld_recv, x_send, x_recv, t_send, t_recv, o_send, o_recv,
           wa_send, wa_recv, wb_send, wb_recv):
    sp, dp, group, cores = sizes
    seqs, heads, seg, width = q_hbm.shape
    stages = sp // group
    own = heads // group
    items = seqs * own
    span = group * seg
    half = width // 2
    rows = ld_hbm.shape[0]
    pairs = dp // cores
    feats = w_hbm.shape[1]

    me = lax.axis_index("sp")
    col = lax.axis_index("dp")
    z, x = lax.div(me, group), lax.rem(me, group)
    pair, core = lax.div(col, cores), lax.rem(col, cores)
    sibling = pair * cores + (cores - 1 - core)
    mine = pl.ds(pl.multiple_of(x * seg, seg), seg)

    barrier = pltpu.get_barrier_semaphore()
    for r in range(1, sp):
        pl.semaphore_signal(barrier, inc=1, device_id={"sp": lax.rem(me + r, sp)}, device_id_type=MESH)
    for r in range(1, pairs):
        pl.semaphore_signal(barrier, inc=1, device_id={"dp": lax.rem(col + cores * r, dp)}, device_id_type=MESH)
    if cores == 2:
        pl.semaphore_signal(barrier, inc=1, device_id={"dp": sibling}, device_id_type=MESH)

    local = [
        pltpu.make_async_copy(ld_hbm, ldbuf.at[me], local_sem.at[0]),
        pltpu.make_async_copy(k_hbm.at[:, pl.ds(x * own, own)], kbuf.at[:, :, mine], local_sem.at[1]),
        pltpu.make_async_copy(v_hbm.at[:, pl.ds(x * own, own)], vbuf.at[:, :, mine], local_sem.at[2]),
        pltpu.make_async_copy(q_hbm.at[:, pl.ds(x * own, own)], qbuf.at[:, :, mine], local_sem.at[3]),
        pltpu.make_async_copy(w_hbm, wbuf.at[col], local_sem.at[4]),
    ]
    for copy in local:
        copy.start()

    def ld_copy(r):
        return pltpu.make_async_remote_copy(
            src_ref=ld_hbm, dst_ref=ldbuf.at[me], send_sem=ld_send.at[r - 1], recv_sem=ld_recv.at[r - 1],
            device_id={"sp": lax.rem(me + r, sp)}, device_id_type=MESH)

    def x_copies(i, r):
        s, hh = lax.div(i, own), lax.rem(i, own)
        to = lax.rem(x + r, group)
        return [
            pltpu.make_async_remote_copy(
                src_ref=src.at[s, to * own + hh], dst_ref=dst.at[s, hh, mine],
                send_sem=x_send.at[n, r - 1, i], recv_sem=x_recv.at[n, r - 1, i],
                device_id={"sp": z * group + to}, device_id_type=MESH)
            for n, (src, dst) in enumerate(((k_hbm, kbuf), (v_hbm, vbuf), (q_hbm, qbuf)))
        ]

    def t_copy(i):
        return pltpu.make_async_remote_copy(
            src_ref=tout.at[i], dst_ref=tin.at[i], send_sem=t_send.at[i], recv_sem=t_recv.at[i],
            device_id={"sp": lax.rem(me + group, sp)}, device_id_type=MESH)

    def o_copy(i, r):
        s, hh = lax.div(i, own), lax.rem(i, own)
        to = lax.rem(x + r, group)
        return pltpu.make_async_remote_copy(
            src_ref=obuf.at[s, hh, pl.ds(pl.multiple_of(to * seg, seg), seg)],
            dst_ref=xbuf.at[pl.ds(pl.multiple_of(s * seg, seg), seg),
                            pl.ds(pl.multiple_of((x * own + hh) * width, width), width)],
            send_sem=o_send.at[r - 1, i], recv_sem=o_recv.at[r - 1, i],
            device_id={"sp": z * group + to}, device_id_type=MESH)

    def wa_copy(r):
        return pltpu.make_async_remote_copy(
            src_ref=w_hbm, dst_ref=wbuf.at[col], send_sem=wa_send.at[r - 1], recv_sem=wa_recv.at[r - 1],
            device_id={"dp": lax.rem(col + cores * r, dp)}, device_id_type=MESH)

    def wb_copy(r):
        shard = lax.rem(pair + pairs - r, pairs) * cores + core
        return pltpu.make_async_remote_copy(
            src_ref=w_hbm if r == 0 else wbuf.at[shard], dst_ref=wbuf.at[shard],
            send_sem=wb_send.at[r], recv_sem=wb_recv.at[r],
            device_id={"dp": sibling}, device_id_type=MESH)

    pl.semaphore_wait(barrier, (sp - 1) + (pairs - 1) + (cores - 1))

    for r in range(1, sp):
        ld_copy(r).start()

    @pl.loop(0, items)
    def _(i):
        for r in range(1, group):
            for copy in x_copies(i, r):
                copy.start()

    for r in range(1, pairs):
        wa_copy(r).start()
    if cores == 2:
        wb_copy(0).start()

    place = lax.broadcasted_iota(jnp.int32, (span, half), 0) + z * span
    angle = place.astype(F32) * freq_ref[...]
    cos_tab[...] = jnp.cos(angle)
    sin_tab[...] = jnp.sin(angle)

    @pl.when(z == 0)
    def _():
        tin[...] = jnp.zeros_like(tin)

    for copy in local[:4]:
        copy.wait()
    for r in range(1, sp):
        ld_copy(r).wait_recv()
    for n in range(sp):
        ldrows[pl.ds(n * rows, rows), :] = ldbuf[n, :, pl.ds(pl.multiple_of(z * span, span), span)]

    def rotate(field):
        wide = field.astype(F32)
        first, second = wide[:, :half], wide[:, half:]
        cosine, sine = cos_tab[...], sin_tab[...]
        return jnp.concatenate(
            [first * cosine - second * sine, second * cosine + first * sine], axis=1).astype(BF16)

    @pl.loop(0, items)
    def _(i):
        s, hh = lax.div(i, own), lax.rem(i, own)
        for r in range(1, group):
            for copy in x_copies(i, r):
                copy.wait_recv()
        rank = lax.broadcasted_iota(jnp.int32, (span, span), 0)
        lane = lax.broadcasted_iota(jnp.int32, (span, span), 1)
        causal = rank >= lane
        decay = ldrows[pl.ds(s * heads + x * own + hh, 1), :]
        within = jnp.sum(jnp.where(causal, decay, 0.0), axis=1, keepdims=True)
        across = jnp.sum(jnp.where(rank == lane, within, 0.0), axis=0, keepdims=True)
        ending = jnp.sum(decay, axis=1, keepdims=True)
        mask = jnp.where(causal, jnp.exp(jnp.where(causal, within - across, 0.0)), 0.0)
        rot_q = rotate(qbuf[s, hh])
        rot_k = rotate(kbuf[s, hh])
        value = vbuf[s, hh]
        scaled = (rot_k.astype(F32) * jnp.exp(jnp.minimum(ending - within, 0.0))).astype(BF16)
        update = lax.dot_general(scaled, value, (((0,), (0,)), ((), ())), preferred_element_type=F32)
        scores = lax.dot_general(rot_q, rot_k, (((1,), (1,)), ((), ())), preferred_element_type=F32)
        weights = (scores * mask).astype(BF16)
        here = jnp.dot(weights, value, preferred_element_type=F32)

        @pl.when(z > 0)
        def _():
            t_copy(i).wait_recv()

        before = tin[i]
        tout[i] = (jnp.exp(ending) * before.astype(F32) + update).astype(BF16)

        @pl.when(z < stages - 1)
        def _():
            t_copy(i).start()

        carried = jnp.dot(rot_q, before, preferred_element_type=F32)
        retained = (here + jnp.exp(within) * carried).astype(BF16).astype(F32)
        square = jnp.mean(retained * retained, axis=1, keepdims=True)
        obuf[s, hh] = (retained * lax.rsqrt(square + 1e-06)).astype(BF16)
        for r in range(1, group):
            o_copy(i, r).start()
        xbuf[pl.ds(pl.multiple_of(s * seg, seg), seg),
             pl.ds(pl.multiple_of((x * own + hh) * width, width), width)] = obuf[s, hh, mine]

    for r in range(1, pairs):
        wa_copy(r).wait_recv()
        if cores == 2:
            wb_copy(r).start()
    local[4].wait()
    if cores == 2:
        for r in range(pairs):
            wb_copy(r).wait_recv()

    @pl.loop(0, items)
    def _(i):
        for r in range(1, group):
            o_copy(i, r).wait_recv()

    @pl.loop(0, dp)
    def _(n):
        out_ref[:, pl.ds(pl.multiple_of(n * feats, feats), feats)] = jnp.dot(
            xbuf[...], wbuf[n], preferred_element_type=F32).astype(BF16)

    for r in range(1, sp):
        ld_copy(r).wait_send()
    for r in range(1, pairs):
        wa_copy(r).wait_send()
    if cores == 2:
        for r in range(pairs):
            wb_copy(r).wait_send()

    @pl.loop(0, items)
    def _(i):
        for r in range(1, group):
            for copy in x_copies(i, r):
                copy.wait_send()
            o_copy(i, r).wait_send()

        @pl.when(z < stages - 1)
        def _():
            t_copy(i).wait_send()


def on_device(sp, dp, queries, keys, values, log_decay, w_out):
    seqs, heads, seg, width = queries.shape
    rows, length = log_decay.shape
    group = 2 if sp % 2 == 0 and heads % 2 == 0 else 1
    cores = 2 if dp % 2 == 0 else 1
    pairs, own = dp // cores, heads // group
    items, span, half = seqs * own, group * seg, width // 2
    feats = w_out.shape[2]
    frequency = (10000.0 ** (-jnp.arange(half, dtype=F32) / half))[None, :]
    dma = pltpu.SemaphoreType.DMA
    some = lambda count: max(count, 1)
    hbm = pl.BlockSpec(memory_space=pl.ANY)
    vmem = pl.BlockSpec(memory_space=pltpu.VMEM)
    mixed = pl.pallas_call(
        functools.partial(kernel, (sp, dp, group, cores)),
        out_shape=jax.ShapeDtypeStruct((seqs * seg, dp * feats), BF16),
        in_specs=[vmem, hbm, hbm, hbm, hbm, hbm],
        out_specs=vmem,
        scratch_shapes=[
            pltpu.VMEM((seqs, own, span, width), BF16),
            pltpu.VMEM((seqs, own, span, width), BF16),
            pltpu.VMEM((seqs, own, span, width), BF16),
            pltpu.VMEM((sp, rows, length), F32),
            pltpu.VMEM((sp * rows, span), F32),
            pltpu.VMEM((span, half), F32),
            pltpu.VMEM((span, half), F32),
            pltpu.VMEM((dp, heads * width, feats), BF16),
            pltpu.VMEM((items, width, width), BF16),
            pltpu.VMEM((items, width, width), BF16),
            pltpu.VMEM((seqs, own, span, width), BF16),
            pltpu.VMEM((seqs * seg, heads * width), BF16),
            dma((5,)),
            dma((some(sp - 1),)), dma((some(sp - 1),)),
            dma((3, some(group - 1), items)), dma((3, some(group - 1), items)),
            dma((items,)), dma((items,)),
            dma((some(group - 1), items)), dma((some(group - 1), items)),
            dma((some(pairs - 1),)), dma((some(pairs - 1),)),
            dma((pairs,)), dma((pairs,)),
        ],
        compiler_params=pltpu.CompilerParams(
            collective_id=0, has_side_effects=True, vmem_limit_bytes=48 * 2**20),
    )(frequency, queries, keys, values, log_decay, w_out.reshape(heads * width, feats))
    return mixed.reshape(seqs, seg, dp * feats)


def solution(mesh):
    placed = (
        P("dp", None, "sp", None),
        P("dp", None, "sp", None),
        P("dp", None, "sp", None),
        P(("dp", "sp"), None),
        P(None, None, "dp"),
    )
    body = functools.partial(on_device, mesh.shape["sp"], mesh.shape["dp"])
    return jax.shard_map(
        body, mesh=mesh, in_specs=placed, out_specs=P("dp", "sp", None), check_vma=False
    )
```

```python
import functools
import math

import jax
import jax.numpy as jnp
from jax import lax
from jax.experimental import pallas as pl
from jax.experimental.pallas import tpu as pltpu
from jax.sharding import PartitionSpec as P

MESH = pl.DeviceIdType.MESH
F32 = jnp.float32
BF16 = jnp.bfloat16


def kernel(sizes, q_hbm, k_hbm, v_hbm, ld_hbm, w_hbm, out_ref,
           qbuf, kbuf, vbuf, ldbuf, ldrows, cos_tab, sin_tab, wbuf, tin, tout, obuf, xbuf,
           ubuf, fall, rkbuf, most,
           local_sem, ld_send, ld_recv, x_send, x_recv, t_send, t_recv, o_send, o_recv,
           wa_send, wa_recv, wb_send, wb_recv):
    sp, dp, group, cores = sizes
    seqs, heads, seg, width = q_hbm.shape
    stages = sp // group
    own = heads // group
    items = seqs * own
    span = group * seg
    half = width // 2
    rows = ld_hbm.shape[0]
    pairs = dp // cores
    feats = w_hbm.shape[1]
    parts = t_send.shape[1]
    slab = width // parts
    cuts = wa_send.shape[1]
    deep = heads * width // cuts

    me = lax.axis_index("sp")
    col = lax.axis_index("dp")
    z, x = lax.div(me, group), lax.rem(me, group)
    pair, core = lax.div(col, cores), lax.rem(col, cores)
    sibling = pair * cores + (cores - 1 - core)
    mine = pl.ds(pl.multiple_of(x * seg, seg), seg)

    barrier = pltpu.get_barrier_semaphore()
    for r in range(1, sp):
        pl.semaphore_signal(barrier, inc=1, device_id={"sp": lax.rem(me + r, sp)}, device_id_type=MESH)
    for r in range(1, pairs):
        pl.semaphore_signal(barrier, inc=1, device_id={"dp": lax.rem(col + cores * r, dp)}, device_id_type=MESH)
    if cores == 2:
        pl.semaphore_signal(barrier, inc=1, device_id={"dp": sibling}, device_id_type=MESH)

    local = [
        pltpu.make_async_copy(ld_hbm, ldbuf.at[me], local_sem.at[0]),
        pltpu.make_async_copy(k_hbm.at[:, pl.ds(x * own, own)], kbuf.at[:, :, mine], local_sem.at[1]),
        pltpu.make_async_copy(v_hbm.at[:, pl.ds(x * own, own)], vbuf.at[:, :, mine], local_sem.at[2]),
        pltpu.make_async_copy(q_hbm.at[:, pl.ds(x * own, own)], qbuf.at[:, :, mine], local_sem.at[3]),
        pltpu.make_async_copy(w_hbm, wbuf.at[col], local_sem.at[4]),
    ]
    for copy in local:
        copy.start()

    def ld_copy(r):
        return pltpu.make_async_remote_copy(
            src_ref=ld_hbm, dst_ref=ldbuf.at[me], send_sem=ld_send.at[r - 1], recv_sem=ld_recv.at[r - 1],
            device_id={"sp": lax.rem(me + r, sp)}, device_id_type=MESH)

    def x_copy(i, r, n):
        s, hh = lax.div(i, own), lax.rem(i, own)
        to = lax.rem(x + r, group)
        src, dst = ((k_hbm, kbuf), (v_hbm, vbuf), (q_hbm, qbuf))[n]
        return pltpu.make_async_remote_copy(
            src_ref=src.at[s, to * own + hh], dst_ref=dst.at[s, hh, mine],
            send_sem=x_send.at[n, r - 1, i], recv_sem=x_recv.at[n, r - 1, i],
            device_id={"sp": z * group + to}, device_id_type=MESH)

    def t_copy(i, p):
        some = pl.ds(p * slab, slab)
        return pltpu.make_async_remote_copy(
            src_ref=tout.at[i, some], dst_ref=tin.at[i, some], send_sem=t_send.at[i, p], recv_sem=t_recv.at[i, p],
            device_id={"sp": lax.rem(me + group, sp)}, device_id_type=MESH)

    def o_copy(i, r):
        s, hh = lax.div(i, own), lax.rem(i, own)
        to = lax.rem(x + r, group)
        return pltpu.make_async_remote_copy(
            src_ref=obuf.at[s, hh, pl.ds(pl.multiple_of(to * seg, seg), seg)],
            dst_ref=xbuf.at[pl.ds(pl.multiple_of(s * seg, seg), seg),
                            pl.ds(pl.multiple_of((x * own + hh) * width, width), width)],
            send_sem=o_send.at[r - 1, i], recv_sem=o_recv.at[r - 1, i],
            device_id={"sp": z * group + to}, device_id_type=MESH)

    def wa_copy(r, c):
        some = pl.ds(c * deep, deep)
        return pltpu.make_async_remote_copy(
            src_ref=w_hbm.at[some], dst_ref=wbuf.at[col, some],
            send_sem=wa_send.at[r - 1, c], recv_sem=wa_recv.at[r - 1, c],
            device_id={"dp": lax.rem(col + cores * r, dp)}, device_id_type=MESH)

    def wb_copy(r, c):
        some = pl.ds(c * deep, deep)
        shard = lax.rem(pair + pairs - r, pairs) * cores + core
        return pltpu.make_async_remote_copy(
            src_ref=w_hbm.at[some] if r == 0 else wbuf.at[shard, some], dst_ref=wbuf.at[shard, some],
            send_sem=wb_send.at[r, c], recv_sem=wb_recv.at[r, c],
            device_id={"dp": sibling}, device_id_type=MESH)

    pl.semaphore_wait(barrier, (sp - 1) + (pairs - 1) + (cores - 1))

    for r in range(1, sp):
        ld_copy(r).start()
    for r in range(1, pairs):
        for c in range(cuts):
            wa_copy(r, c).start()

    @pl.loop(0, items)
    def _(i):
        for r in range(1, group):
            for n in range(3):
                x_copy(i, r, n).start()

    if cores == 2:
        for c in range(cuts):
            wb_copy(0, c).start()

    place = lax.broadcasted_iota(jnp.int32, (span, half), 0) + z * span
    order = lax.broadcasted_iota(jnp.int32, (1, half), 1).astype(F32)
    angle = place.astype(F32) * jnp.exp(order * (-math.log(10000.0) / half))
    cos_tab[...] = jnp.cos(angle)
    sin_tab[...] = jnp.sin(angle)

    @pl.when(z == 0)
    def _():
        tin[...] = jnp.zeros_like(tin)

    for copy in local[:4]:
        copy.wait()
    for r in range(1, sp):
        ld_copy(r).wait_recv()
    for n in range(sp):
        ldrows[pl.ds(n * rows, rows), :] = ldbuf[n, :, pl.ds(pl.multiple_of(z * span, span), span)]

    def rotate(field):
        wide = field.astype(F32)
        first, second = wide[:, :half], wide[:, half:]
        cosine, sine = cos_tab[...], sin_tab[...]
        return jnp.concatenate(
            [first * cosine - second * sine, second * cosine + first * sine], axis=1).astype(BF16)

    rank = lax.broadcasted_iota(jnp.int32, (span, span), 0)
    lane = lax.broadcasted_iota(jnp.int32, (span, span), 1)

    def decays(s, hh):
        decay = ldrows[pl.ds(s * heads + x * own + hh, 1), :]
        return decay, jnp.sum(jnp.where(rank >= lane, decay, 0.0), axis=1, keepdims=True)

    def prepare(i):
        s, hh, slot = lax.div(i, own), lax.rem(i, own), lax.rem(i, 2)
        for r in range(1, group):
            for n in range(2):
                x_copy(i, r, n).wait_recv()
        decay, within = decays(s, hh)
        ending = jnp.sum(decay, axis=1, keepdims=True)
        rot_k = rotate(kbuf[s, hh])
        rkbuf[slot] = rot_k
        scaled = (rot_k.astype(F32) * jnp.exp(jnp.minimum(ending - within, 0.0))).astype(BF16)
        fall[slot] = jnp.broadcast_to(jnp.exp(ending), fall.shape[1:])
        ubuf[slot] = lax.dot_general(
            scaled, vbuf[s, hh], (((0,), (0,)), ((), ())), preferred_element_type=F32)

    def advance(i):
        slot = lax.rem(i, 2)
        factor = fall[slot, 0:1, :]
        for p in range(parts):
            @pl.when(z > 0)
            def _():
                t_copy(i, p).wait_recv()

            @pl.when(z < stages - 1)
            def _():
                some = pl.ds(p * slab, slab)
                tout[i, some] = (factor * tin[i, some].astype(F32) + ubuf[slot, some]).astype(BF16)
                t_copy(i, p).start()

    def attend(i):
        s, hh, slot = lax.div(i, own), lax.rem(i, own), lax.rem(i, 2)
        for r in range(1, group):
            x_copy(i, r, 2).wait_recv()
        _, within = decays(s, hh)
        across = jnp.sum(jnp.where(rank == lane, within, 0.0), axis=0, keepdims=True)
        causal = rank >= lane
        mask = jnp.where(causal, jnp.exp(jnp.where(causal, within - across, 0.0)), 0.0)
        rot_q = rotate(qbuf[s, hh])
        scores = lax.dot_general(rot_q, rkbuf[slot], (((1,), (1,)), ((), ())), preferred_element_type=F32)
        weights = (scores * mask).astype(BF16)
        here = jnp.dot(weights, vbuf[s, hh], preferred_element_type=F32)
        carried = jnp.dot(rot_q, tin[i], preferred_element_type=F32)
        retained = (here + jnp.exp(within) * carried).astype(BF16).astype(F32)
        square = jnp.mean(retained * retained, axis=1, keepdims=True)
        obuf[s, hh] = (retained * lax.rsqrt(square + 1e-06)).astype(BF16)
        for r in range(1, group):
            o_copy(i, r).start()
        xbuf[pl.ds(pl.multiple_of(s * seg, seg), seg),
             pl.ds(pl.multiple_of((x * own + hh) * width, width), width)] = obuf[s, hh, mine]

    def pass_w(c):
        for r in range(1, pairs):
            wa_copy(r, c).wait_recv()
            if cores == 2:
                wb_copy(r, c).start()

    def land(first, last):
        @pl.loop(first, last)
        def _(i):
            for r in range(1, group):
                o_copy(i, r).wait_recv()

    def project(first, count):
        land(first * own, (first + count) * own)
        if count:
            some = pl.ds(first * seg, count * seg)

            @pl.loop(0, dp)
            def _(n):
                out_ref[some, pl.ds(pl.multiple_of(n * feats, feats), feats)] = jnp.dot(
                    xbuf[some, :], wbuf[n], preferred_element_type=F32).astype(BF16)

    final = pl.ds((seqs - 1) * seg, seg)

    def heads_of(first, count, n):
        total = jnp.zeros((seg, feats), F32)
        for g in range(group if count else 0):
            some = pl.ds((g * own + first) * width, count * width)
            total = total + jnp.dot(xbuf[final, some], wbuf[n, some, :], preferred_element_type=F32)
        return total

    def most_of_final():
        land((seqs - 1) * own, items - 1)

        @pl.loop(0, dp)
        def _(n):
            most[n] = heads_of(0, own - 1, n)

    def rest_of_final():
        land(items - 1, items)

        @pl.loop(0, dp)
        def _(n):
            out_ref[final, pl.ds(pl.multiple_of(n * feats, feats), feats)] = (
                most[n] + heads_of(own - 1, 1, n)).astype(BF16)

    def whole_w():
        pass_w(cuts - 1)
        local[4].wait()
        if cores == 2:
            for r in range(pairs):
                for c in range(cuts):
                    wb_copy(r, c).wait_recv()

    hold = items * 3 // 4
    prepare(0)

    def turn(i):
        advance(i)
        attend(i)

        @pl.when(i + 1 < items)
        def _():
            prepare(i + 1)

    @pl.loop(0, hold)
    def _(i):
        turn(i)

    for c in range(cuts - 1):
        pass_w(c)

    @pl.loop(hold, items - 2)
    def _(i):
        turn(i)

    early = max(seqs - 2, 0)

    @pl.when(z == stages - 1)
    def _():
        whole_w()
        project(0, early)

    turn(items - 2)

    @pl.when(z == stages - 1)
    def _():
        project(early, seqs - 1 - early)

    turn(items - 1)

    @pl.when(z < stages - 1)
    def _():
        whole_w()
        project(0, seqs - 1)

    most_of_final()
    rest_of_final()

    for r in range(1, sp):
        ld_copy(r).wait_send()
    for c in range(cuts):
        for r in range(1, pairs):
            wa_copy(r, c).wait_send()
        if cores == 2:
            for r in range(pairs):
                wb_copy(r, c).wait_send()

    @pl.loop(0, items)
    def _(i):
        for r in range(1, group):
            for n in range(3):
                x_copy(i, r, n).wait_send()
            o_copy(i, r).wait_send()

        @pl.when(z < stages - 1)
        def _():
            for p in range(parts):
                t_copy(i, p).wait_send()


def on_device(sp, dp, queries, keys, values, log_decay, w_out):
    seqs, heads, seg, width = queries.shape
    rows, length = log_decay.shape
    group = 2 if sp % 2 == 0 and heads % 2 == 0 else 1
    cores = 2 if dp % 2 == 0 else 1
    pairs, own = dp // cores, heads // group
    items, span, half = seqs * own, group * seg, width // 2
    feats = w_out.shape[2]
    parts, cuts = 4, 2
    dma = pltpu.SemaphoreType.DMA
    some = lambda count: max(count, 1)
    hbm = pl.BlockSpec(memory_space=pl.ANY)
    vmem = pl.BlockSpec(memory_space=pltpu.VMEM)
    mixed = pl.pallas_call(
        functools.partial(kernel, (sp, dp, group, cores)),
        out_shape=jax.ShapeDtypeStruct((seqs * seg, dp * feats), BF16),
        in_specs=[hbm, hbm, hbm, hbm, hbm],
        out_specs=vmem,
        scratch_shapes=[
            pltpu.VMEM((seqs, own, span, width), BF16),
            pltpu.VMEM((seqs, own, span, width), BF16),
            pltpu.VMEM((seqs, own, span, width), BF16),
            pltpu.VMEM((sp, rows, length), F32),
            pltpu.VMEM((sp * rows, span), F32),
            pltpu.VMEM((span, half), F32),
            pltpu.VMEM((span, half), F32),
            pltpu.VMEM((dp, heads * width, feats), BF16),
            pltpu.VMEM((items, width, width), BF16),
            pltpu.VMEM((items, width, width), BF16),
            pltpu.VMEM((seqs, own, span, width), BF16),
            pltpu.VMEM((seqs * seg, heads * width), BF16),
            pltpu.VMEM((2, width, width), F32),
            pltpu.VMEM((2, 8, width), F32),
            pltpu.VMEM((2, span, width), BF16),
            pltpu.VMEM((dp, seg, feats), F32),
            dma((5,)),
            dma((some(sp - 1),)), dma((some(sp - 1),)),
            dma((3, some(group - 1), items)), dma((3, some(group - 1), items)),
            dma((items, parts)), dma((items, parts)),
            dma((some(group - 1), items)), dma((some(group - 1), items)),
            dma((some(pairs - 1), cuts)), dma((some(pairs - 1), cuts)),
            dma((pairs, cuts)), dma((pairs, cuts)),
        ],
        compiler_params=pltpu.CompilerParams(
            collective_id=0, has_side_effects=True, vmem_limit_bytes=67043328),
    )(queries, keys, values, log_decay, w_out.reshape(heads * width, feats))
    return mixed.reshape(seqs, seg, dp * feats)


def solution(mesh):
    placed = (
        P("dp", None, "sp", None),
        P("dp", None, "sp", None),
        P("dp", None, "sp", None),
        P(("dp", "sp"), None),
        P(None, None, "dp"),
    )
    body = functools.partial(on_device, mesh.shape["sp"], mesh.shape["dp"])
    return jax.shard_map(
        body, mesh=mesh, in_specs=placed, out_specs=P("dp", "sp", None), check_vma=False
    )
```
